32 devices in a mesh: sp: 8 (over z, x), tp: 4 (over y, core).
Axes of the slice: x: 2, y: 2, z: 4, core: 2. Of those that a mesh axis runs over, the one named last changes fastest.
Arguments:
- features: bfloat16 [3072, 2048], P('sp', 'tp'), may hold values from -6 to 6
- norm_gain: float32 [2048], replicated, may hold values from 0.28 to 10
- w_query: bfloat16 [2048, 1024], P(None, 'tp'), may hold values from -0.125 to 0.125
- w_key: bfloat16 [2048, 512], P(None, 'tp'), may hold values from -0.125 to 0.125
- w_value: bfloat16 [2048, 512], P(None, 'tp'), may hold values from -0.125 to 0.125
- head_sinks: float32 [16], P('tp'), may hold values from 1 to 5
- w_query_latent: bfloat16 [2048, 512], replicated, may hold values from -0.125 to 0.125
- w_kv_latent: bfloat16 [2048, 512], replicated, may hold values from -0.125 to 0.125
- w_rope_key: bfloat16 [2048, 64], replicated, may hold values from -0.125 to 0.125
- query_latent_gain: float32 [512], replicated, may hold values from 0.28 to 10
- kv_latent_gain: float32 [512], replicated, may hold values from 0.28 to 10
- w_query_content: bfloat16 [512, 1024], P(None, 'tp'), may hold values from -0.25 to 0.25
- w_query_rotary: bfloat16 [512, 512], P(None, 'tp'), may hold values from -0.25 to 0.25
- w_key_up: bfloat16 [512, 1024], P(None, 'tp'), may hold values from -0.25 to 0.25
- w_value_up: bfloat16 [512, 1024], P(None, 'tp'), may hold values from -0.25 to 0.25
- w_branch_window: bfloat16 [1024, 2048], P('tp'), may hold values from -0.1875 to 0.1875
- w_branch_latent: bfloat16 [1024, 2048], P('tp'), may hold values from -0.1875 to 0.1875
- w_gate_window: bfloat16 [2048, 2048], P(None, 'tp'), may hold values from -0.125 to 0.125
- w_gate_latent: bfloat16 [2048, 2048], P(None, 'tp'), may hold values from -0.125 to 0.125
Outputs:
- mixed: bfloat16 [3072, 2048], P('sp', 'tp')
The draws below stay inside these ranges and needn't reach their ends.
All inputs are finite; a program needn't handle non-finite values.
Results may differ from the reference program's by a relative error of at most 0.018.
The reference program's roundings to bfloat16 on the way count: a program that leaves them out, or rounds other values in their place, can miss the bound.
Values may be sent and summed in bfloat16 or wider, within the bound.
A program may use at most 128 MiB of HBM per device.

```python
import jax
import jax.numpy as jnp
from jax import lax

D = 2048
Q_HEADS = 16
KV_HEADS = 8
HEAD = 64
WINDOW = 128
LAT_HEADS = 8
Q_LATENT = 512
KV_LATENT = 512
NOPE = 128
ROPE = 64
VDIM = 128
TOK_DEV = 384
SEQ = 3072


def gain_draw(key, length):
    return 1.0 + 0.18 * jnp.clip(jax.random.normal(key, (length,), jnp.float32), -4.0, 4.0)


def draw_norm_gain(key, part):
    return gain_draw(jax.random.fold_in(key, 11), D)


def draw_query_latent_gain(key, part):
    return gain_draw(jax.random.fold_in(key, 23), Q_LATENT)


def draw_kv_latent_gain(key, part):
    return gain_draw(jax.random.fold_in(key, 37), KV_LATENT)


def block_levels(stream_key, extent, cuts, smallest, top_value):
    def one(axis_at, blocks):
        steps = jax.random.uniform(jax.random.fold_in(jax.random.fold_in(stream_key, 6), axis_at), (blocks,), jnp.float32, smallest / len(cuts), top_value / len(cuts))
        return jnp.repeat(jnp.exp(steps), extent[axis_at] // blocks).reshape((-1,) + (1,) * (len(extent) - axis_at - 1))

    loudness = one(*cuts[0])
    for cut in cuts[1:]:
        loudness = loudness * one(*cut)
    return loudness


def normal_values(stream_key, dims, width, reach, pieces=(), kind=jnp.bfloat16):
    loudness = block_levels(stream_key, dims, pieces, -0.22, 0.18) if pieces else 1.0
    values = jax.random.normal(stream_key, dims, jnp.float32) * width * loudness
    return jnp.minimum(jnp.maximum(values, -reach), reach).astype(kind)


def setup_inputs(seed: int = 0) -> dict:
    key_of = jax.random.split(jax.random.key(seed), 20)
    return {
        "features": normal_values(key_of[0], (SEQ, D), 1.0, 6.0, ((0, 8), (1, 4))),
        "norm_gain": draw_norm_gain(jax.random.fold_in(key_of[19], 71), 0),
        "w_query": normal_values(key_of[2], (D, Q_HEADS * HEAD), D ** -0.5, 0.125, ((1, 4),)),
        "w_key": normal_values(key_of[3], (D, KV_HEADS * HEAD), D ** -0.5, 0.125, ((1, 4),)),
        "w_value": normal_values(key_of[4], (D, KV_HEADS * HEAD), D ** -0.5, 0.125, ((1, 4),)),
        "head_sinks": jnp.clip(1.0 + 4.0 * jax.random.uniform(key_of[5], (Q_HEADS,), jnp.float32) ** block_levels(key_of[5], (Q_HEADS,), ((0, 4),), -0.2, 0.2), 1.0, 5.0),
        "w_query_latent": normal_values(key_of[6], (D, Q_LATENT), D ** -0.5, 0.125),
        "w_kv_latent": normal_values(key_of[7], (D, KV_LATENT), D ** -0.5, 0.125),
        "w_rope_key": normal_values(key_of[8], (D, ROPE), D ** -0.5, 0.125),
        "query_latent_gain": draw_query_latent_gain(jax.random.fold_in(key_of[19], 71), 0),
        "kv_latent_gain": draw_kv_latent_gain(jax.random.fold_in(key_of[19], 71), 0),
        "w_query_content": normal_values(key_of[11], (Q_LATENT, LAT_HEADS * NOPE), Q_LATENT ** -0.5, 0.25, ((1, 4),)),
        "w_query_rotary": normal_values(key_of[12], (Q_LATENT, LAT_HEADS * ROPE), Q_LATENT ** -0.5, 0.25, ((1, 4),)),
        "w_key_up": normal_values(key_of[13], (KV_LATENT, LAT_HEADS * NOPE), KV_LATENT ** -0.5, 0.25, ((1, 4),)),
        "w_value_up": normal_values(key_of[14], (KV_LATENT, LAT_HEADS * VDIM), KV_LATENT ** -0.5, 0.25, ((1, 4),)),
        "w_branch_window": normal_values(key_of[15], (Q_HEADS * HEAD, D), (Q_HEADS * HEAD) ** -0.5, 0.1875, ((0, 4),)),
        "w_branch_latent": normal_values(key_of[16], (LAT_HEADS * VDIM, D), (LAT_HEADS * VDIM) ** -0.5, 0.1875, ((0, 4),)),
        "w_gate_window": normal_values(key_of[17], (D, D), D ** -0.5, 0.125, ((1, 4),)),
        "w_gate_latent": normal_values(key_of[18], (D, D), D ** -0.5, 0.125, ((1, 4),)),
    }


EPS = 1e-06
THETA = 10000.0
NEGATIVE = -1e+30

def rms_rows(float_rows, gain_vec):
    return float_rows * lax.rsqrt(lax.optimization_barrier(jnp.mean(float_rows * float_rows, axis=-1, keepdims=True)) + EPS) * gain_vec

def rotate(float_rows, positions):
    half_width = float_rows.shape[-1] // 2
    frequencies = THETA ** (-jnp.arange(half_width, dtype=jnp.float32) / half_width)
    angles = positions.astype(jnp.float32)[:, None] * frequencies
    target = (float_rows.shape[0],) + (1,) * (float_rows.ndim - 2) + (half_width,)
    cosine = jnp.cos(angles).reshape(target)
    sine_part = jnp.sin(angles).reshape(target)
    first_half = float_rows[..., :half_width]
    second_half = float_rows[..., half_width:]
    return jnp.concatenate([first_half * cosine - second_half * sine_part, second_half * cosine + first_half * sine_part], axis=-1)

def window_attention(queries, key_ext, value_ext, sink_table, row_start):
    row_count = queries.shape[0]
    kv_heads = key_ext.shape[1] // HEAD
    group_size = queries.shape[1] // HEAD // kv_heads
    blocks = row_count // WINDOW
    query_blocks = queries.reshape(blocks, WINDOW, kv_heads, group_size, HEAD).astype(jnp.float32)

    def banded(table):
        table = table.reshape(blocks + 1, WINDOW, kv_heads, HEAD)
        return jnp.concatenate([table[:-1], table[1:]], axis=1).astype(jnp.float32)
    key_band = banded(key_ext)
    value_band = banded(value_ext)
    scores = jnp.einsum('nqhgd,nkhd->nhgqk', query_blocks, key_band) * HEAD ** (-0.5)
    query_index = jnp.arange(WINDOW, dtype=jnp.int32)[:, None]
    key_index = jnp.arange(2 * WINDOW, dtype=jnp.int32)[None, :]
    offset = query_index + WINDOW - key_index
    key_position = row_start + jnp.arange(blocks, dtype=jnp.int32)[:, None, None] * WINDOW + key_index - WINDOW
    valid_mask = ((offset >= 0) & (offset < WINDOW) & (key_position >= 0))[:, None, None]
    scores = jnp.where(valid_mask, scores, NEGATIVE)
    sink_logit = sink_table.reshape(1, kv_heads, group_size, 1, 1)
    row_top = jnp.maximum(lax.optimization_barrier(jnp.max(scores, axis=-1, keepdims=True)), sink_logit)
    weights = jnp.where(valid_mask, jnp.exp(scores - row_top), 0.0)
    denominator = lax.optimization_barrier(jnp.sum(weights, axis=-1, keepdims=True)) + jnp.exp(sink_logit - row_top)
    probabilities = (weights / denominator).astype(jnp.bfloat16).astype(jnp.float32)
    attended = jnp.einsum('nhgqk,nkhd->nqhgd', probabilities, value_band)
    return attended.astype(jnp.bfloat16).reshape(row_count, kv_heads * group_size * HEAD)

def latent_attention(query_content, query_rotary, head_keys, head_values, rope_key):
    seq_rows = query_content.shape[0]
    lat_heads = query_content.shape[1]
    blocks = seq_rows // TOK_DEV
    scale_factor = (NOPE + ROPE) ** (-0.5)
    key_float = head_keys.astype(jnp.float32)
    value_float = head_values.astype(jnp.float32)
    rope_float = rope_key.astype(jnp.float32)
    content_blocks = query_content.reshape(blocks, TOK_DEV, lat_heads, NOPE)
    rotary_blocks = query_rotary.reshape(blocks, TOK_DEV, lat_heads, ROPE)
    key_position = jnp.arange(seq_rows, dtype=jnp.int32)

    def one_block(inputs):
        content_part, rotary_part, block_index = inputs
        scores = (jnp.einsum('qhd,khd->hqk', content_part.astype(jnp.float32), key_float) + jnp.einsum('qhr,kr->hqk', rotary_part.astype(jnp.float32), rope_float)) * scale_factor
        query_position = block_index * TOK_DEV + jnp.arange(TOK_DEV, dtype=jnp.int32)
        live_mask = key_position[None, :] <= query_position[:, None]
        scores = jnp.where(live_mask, scores, NEGATIVE)
        row_top = lax.optimization_barrier(jnp.max(scores, axis=-1, keepdims=True))
        weights = jnp.where(live_mask, jnp.exp(scores - row_top), 0.0)
        rounded = weights.astype(jnp.bfloat16).astype(jnp.float32)
        attended = jnp.einsum('hqk,khd->qhd', rounded, value_float)
        denominator = jnp.transpose(lax.optimization_barrier(jnp.sum(weights, axis=-1)))[:, :, None]
        return (attended / denominator).astype(jnp.bfloat16)
    result = lax.map(one_block, (content_blocks, rotary_blocks, jnp.arange(blocks, dtype=jnp.int32)))
    return result.reshape(seq_rows, lat_heads * VDIM)

def project(left, right):
    return jnp.dot(left, right, preferred_element_type=jnp.float32)

def reference(features, norm_gain, w_query, w_key, w_value, head_sinks, w_query_latent, w_kv_latent, w_rope_key, query_latent_gain, kv_latent_gain, w_query_content, w_query_rotary, w_key_up, w_value_up, w_branch_window, w_branch_latent, w_gate_window, w_gate_latent):
    seq_rows = features.shape[0]
    positions = jnp.arange(seq_rows, dtype=jnp.int32)
    normed = rms_rows(features.astype(jnp.float32), norm_gain).astype(jnp.bfloat16)
    query_rows = project(normed, w_query).astype(jnp.bfloat16)
    key_rows = project(normed, w_key).astype(jnp.bfloat16)
    value_rows = project(normed, w_value).astype(jnp.bfloat16)
    padding = jnp.zeros((WINDOW, key_rows.shape[1]), jnp.bfloat16)
    window_out = window_attention(query_rows, jnp.concatenate([padding, key_rows], axis=0), jnp.concatenate([padding, value_rows], axis=0), head_sinks, 0)
    latent_query = rms_rows(project(normed, w_query_latent), query_latent_gain).astype(jnp.bfloat16)
    latent_kv = rms_rows(project(normed, w_kv_latent), kv_latent_gain).astype(jnp.bfloat16)
    rope_key = rotate(project(normed, w_rope_key), positions).astype(jnp.bfloat16)
    query_content = project(latent_query, w_query_content).astype(jnp.bfloat16).reshape(seq_rows, LAT_HEADS, NOPE)
    query_rotary = rotate(project(latent_query, w_query_rotary).reshape(seq_rows, LAT_HEADS, ROPE), positions).astype(jnp.bfloat16)
    head_keys = project(latent_kv, w_key_up).astype(jnp.bfloat16).reshape(seq_rows, LAT_HEADS, NOPE)
    head_values = project(latent_kv, w_value_up).astype(jnp.bfloat16).reshape(seq_rows, LAT_HEADS, VDIM)
    latent_out = latent_attention(query_content, query_rotary, head_keys, head_values, rope_key)
    window_branch = project(window_out, w_branch_window)
    latent_branch = project(latent_out, w_branch_latent)
    window_gate = jax.nn.sigmoid(project(normed, w_gate_window))
    latent_gate = jax.nn.sigmoid(project(normed, w_gate_latent))
    return (window_gate * window_branch + latent_gate * latent_branch).astype(jnp.bfloat16)
```

```python
import functools

import jax
import jax.numpy as jnp
from jax import lax
from jax.experimental import pallas as pl
from jax.experimental.pallas import tpu as pltpu
from jax.sharding import PartitionSpec as P

HEAD = 64
WINDOW = 128
NOPE = 128
ROPE = 64
VDIM = 128


EPS = 1e-06
THETA = 10000.0
NEGATIVE = -1e30
LANES = 128
MESH = pl.DeviceIdType.MESH
BF16 = jnp.bfloat16
F32 = jnp.float32


def dot(left, right):
    return jnp.dot(left, right, preferred_element_type=F32)


def dot_t(left, right):
    return lax.dot_general(left, right, (((1,), (1,)), ((), ())), preferred_element_type=F32)


def rms_rows(rows, gain):
    return rows * lax.rsqrt(jnp.mean(rows * rows, axis=-1, keepdims=True) + EPS) * gain


def swap_halves(rows):
    half = rows.shape[1] // 2
    return jnp.concatenate([rows[:, half:], rows[:, :half]], axis=1)


WEIGHTS = (
    "kv_latent", "rope", "key", "value", "query", "query_latent", "content", "rotary",
    "key_up", "value_up", "gate_window", "gate_latent",
)


def kernel(dims, *refs):
    n_sp, n_tp, n_x = dims
    n_z, n_y = n_sp // n_x, n_tp // 2
    features, norm_gain, sinks, q_gain, kv_gain, cosine, sine = refs[:7]
    w_hbm = dict(zip(WEIGHTS, refs[7:19]))
    branch_hbm = refs[19:21]
    out = refs[21]
    feat, normed, wide = refs[22:25]
    w = dict(zip(WEIGHTS, refs[25:37]))
    columns = refs[37:39]
    kvb, local_kv, halo, queries, q_full, gates, win, lat, top, total, acc = refs[39:50]
    w_sem, own_sem, col_own, col_send, col_recv, halo_sem, y_send, y_recv, s_send, s_recv = refs[50:60]
    z_send, z_recv, x_send, x_recv, c_send, c_recv, d_send, d_recv = refs[60:68]

    sp, tp = lax.axis_index("sp"), lax.axis_index("tp")
    z, x = sp // n_x, lax.rem(sp, n_x)
    y, core = tp // 2, lax.rem(tp, 2)
    sibling = y * 2 + (1 - core)
    rows, block = features.shape
    half = rows // 2
    lat_heads = w_hbm["key_up"].shape[1] // NOPE
    kv_width = w_hbm["key"].shape[1]
    kv_heads = kv_width // HEAD
    group = w_hbm["query"].shape[1] // kv_width
    latent = w_hbm["kv_latent"].shape[1]

    loads = {}
    own_feat = pltpu.make_async_copy(features, feat.at[tp], own_sem.at[0])
    own_feat.start()
    for i, name in enumerate(WEIGHTS):
        loads[name] = pltpu.make_async_copy(w_hbm[name], w[name], w_sem.at[i])
        loads[name].start()

    def remote(src, dst, send, recv, where):
        return pltpu.make_async_remote_copy(
            src_ref=src, dst_ref=dst, send_sem=send, recv_sem=recv,
            device_id=where, device_id_type=MESH,
        )

    barrier = pltpu.get_barrier_semaphore()

    def greet(where):
        pl.semaphore_signal(barrier, inc=1, device_id=where, device_id_type=MESH)

    for d in range(1, n_tp):
        greet({"sp": sp, "tp": lax.rem(tp + d, n_tp)})
    for d in range(1, n_x):
        greet({"sp": z * n_x + lax.rem(x + d, n_x), "tp": tp})

    @pl.when(z + 1 < n_z)
    def _():
        greet({"sp": sp + n_x, "tp": tp})

    @pl.when(z > 0)
    def _():
        greet({"sp": sp - n_x, "tp": tp})

    @pl.when(sp + 1 < n_sp)
    def _():
        greet({"sp": sp + 1, "tp": tp})

    @pl.when(sp > 0)
    def _():
        greet({"sp": sp - 1, "tp": tp})

    one, none = jnp.int32(1), jnp.int32(0)
    pl.semaphore_wait(
        barrier,
        n_tp - 1 + n_x - 1
        + jnp.where(z + 1 < n_z, one, none) + jnp.where(z > 0, one, none)
        + jnp.where(sp + 1 < n_sp, one, none) + jnp.where(sp > 0, one, none),
    )

    def gather(buf, which):
        own = buf.at[tp]
        sends = [
            remote(own, own, y_send.at[which, d], y_recv.at[which, d],
                   {"sp": sp, "tp": lax.rem(y + d, n_y) * 2 + core})
            for d in range(1, n_y)
        ]
        sends.append(remote(own, own, s_send.at[which, 0], s_recv.at[which, 0],
                            {"sp": sp, "tp": sibling}))
        return sends

    def start(copies):
        for copy in copies:
            copy.start()

    def arrived(buf, which):
        for d in range(1, n_y):
            slot = lax.rem(y + n_y - d, n_y) * 2 + core
            ref = buf.at[slot]
            remote(ref, ref, y_send.at[which, d], y_recv.at[which, d],
                   {"sp": sp, "tp": sibling}).wait_recv()
            remote(ref, ref, s_send.at[which, d], s_recv.at[which, d],
                   {"sp": sp, "tp": sibling}).start()
        for d in range(n_y):
            ref = buf.at[lax.rem(y + n_y - d, n_y) * 2 + (1 - core)]
            remote(ref, ref, s_send.at[which, d], s_recv.at[which, d],
                   {"sp": sp, "tp": sibling}).wait_recv()

    def sent(buf, which):
        own = buf.at[tp]
        for d in range(1, n_y):
            remote(own, own, y_send.at[which, d], y_recv.at[which, d],
                   {"sp": sp, "tp": sibling}).wait_send()
        for d in range(n_y):
            remote(own, own, s_send.at[which, d], s_recv.at[which, d],
                   {"sp": sp, "tp": sibling}).wait_send()

    own_feat.wait()
    start(gather(feat, 0))
    arrived(feat, 0)

    def column_copies():
        local, sends = [], []
        for b in range(2):
            span = branch_hbm[b]
            local.append(pltpu.make_async_copy(
                span.at[:, pl.ds(pl.multiple_of(tp * block, LANES), block)],
                columns[b].at[tp], col_own.at[b]))
            for d in range(1, n_tp):
                to = lax.rem(tp + d, n_tp)
                sends.append(remote(
                    span.at[:, pl.ds(pl.multiple_of(to * block, LANES), block)],
                    columns[b].at[tp], col_send.at[b, d], col_recv.at[b, d],
                    {"sp": sp, "tp": to}))
        return local, sends

    column_local, column_sends = column_copies()
    start(column_local)
    start(column_sends)

    squares = jnp.zeros((rows, 1), F32)
    for j in range(n_tp):
        piece = feat[j].astype(F32)
        squares = squares + jnp.sum(piece * piece, axis=-1, keepdims=True)
    scale = lax.rsqrt(squares / (n_tp * block) + EPS)
    for j in range(n_tp):
        span = slice(j * block, (j + 1) * block)
        normed[:, span] = (feat[j].astype(F32) * scale * norm_gain[:, span]).astype(BF16)

    def wide_dot(name):
        loads[name].wait()
        tile = min(256, latent)

        def step(i, _):
            at = pl.ds(pl.multiple_of(i * tile, LANES), tile)
            wide[:, at] = dot(normed[...], w[name][:, at])
            return 0

        lax.fori_loop(0, w[name].shape[1] // tile, step, 0)

    wide_dot("kv_latent")
    latents = rms_rows(wide[...], kv_gain[...]).astype(BF16)
    loads["rope"].wait()
    rope = dot(normed[...], w["rope"][...])
    rope = rope * cosine[...] + swap_halves(rope) * sine[...]
    padding = jnp.zeros((rows, LANES - ROPE), F32)
    rope = jnp.concatenate([rope, padding], axis=1).astype(BF16)
    kvb[sp, :, :, :latent] = latents.reshape(2, half, latent)
    kvb[sp, :, :, latent:] = rope.reshape(2, half, LANES)

    def column_slot(k):
        return (z - k) * n_x + x

    def z_copy(k):
        ref = kvb.at[column_slot(k), core]
        return remote(ref, ref, z_send.at[k], z_recv.at[k + 1], {"sp": sp + n_x, "tp": tp})

    def x_copy(k, d):
        ref = kvb.at[column_slot(k), core]
        return remote(ref, ref, x_send.at[k, d], x_recv.at[k, d],
                      {"sp": z * n_x + lax.rem(x + d, n_x), "tp": tp})

    def c_copy(k, which):
        ref = kvb.at[column_slot(k), which]
        return remote(ref, ref, c_send.at[k], c_recv.at[k], {"sp": sp, "tp": sibling})

    def row_slot(k, d):
        return (z - k) * n_x + lax.rem(x + n_x - d, n_x)

    def d_copy(k, d, which):
        ref = kvb.at[row_slot(k, d), which]
        return remote(ref, ref, d_send.at[k, d], d_recv.at[k, d], {"sp": sp, "tp": sibling})

    def pass_on(k):
        @pl.when(z + 1 < n_z)
        def _():
            z_copy(k).start()

        for d in range(1, n_x):
            x_copy(k, d).start()

    def take_column(k):
        ref = kvb.at[column_slot(k), core]
        remote(ref, ref, z_send.at[k], z_recv.at[k], {"sp": sp, "tp": sibling}).wait_recv()
        pass_on(k)
        c_copy(k, core).start()

    def take_rows(k):
        for d in range(1, n_x):
            ref = kvb.at[row_slot(k, d), core]
            remote(ref, ref, x_send.at[k, d], x_recv.at[k, d],
                   {"sp": sp, "tp": sibling}).wait_recv()
            d_copy(k, d, core).start()

    pass_on(0)

    loads["key"].wait()
    loads["value"].wait()
    local_kv[:, :kv_width] = dot(normed[...], w["key"][...]).astype(BF16)
    local_kv[:, kv_width:] = dot(normed[...], w["value"][...]).astype(BF16)
    tail = local_kv.at[pl.ds(rows - WINDOW, WINDOW)]
    halo_copy = remote(tail, halo, halo_sem.at[0], halo_sem.at[1], {"sp": sp + 1, "tp": tp})

    @pl.when(sp + 1 < n_sp)
    def _():
        halo_copy.start()

    loads["query"].wait()
    queries[...] = dot(normed[...], w["query"][...]).astype(BF16)

    wide_dot("query_latent")
    latent_query = rms_rows(wide[...], q_gain[...]).astype(BF16)
    loads["content"].wait()
    loads["rotary"].wait()
    content = dot(latent_query, w["content"][...]).astype(BF16)
    rotary = dot(latent_query, w["rotary"][...])
    for h in range(lat_heads):
        turned = rotary[:, h * ROPE : (h + 1) * ROPE]
        turned = turned * cosine[...] + swap_halves(turned) * sine[...]
        q_full[h, :, :NOPE] = content[:, h * NOPE : (h + 1) * NOPE]
        q_full[h, :, NOPE:] = jnp.concatenate([turned, padding], axis=1).astype(BF16)
    loads["key_up"].wait()
    loads["value_up"].wait()

    def attend(slot, diagonal):
        both = kvb[slot].reshape(rows, latent + LANES)
        source, rope_part = both[:, :latent], both[:, latent:]
        keys = dot(source, w["key_up"][...]).astype(BF16)
        values = dot(source, w["value_up"][...]).astype(BF16)
        for h in range(lat_heads):
            key = jnp.concatenate([keys[:, h * NOPE : (h + 1) * NOPE], rope_part], axis=1)
            scores = dot_t(q_full[h], key) * (NOPE + ROPE) ** (-0.5)
            if diagonal:
                live = (lax.broadcasted_iota(jnp.int32, scores.shape, 1)
                        <= lax.broadcasted_iota(jnp.int32, scores.shape, 0))
                scores = jnp.where(live, scores, NEGATIVE)
            peak = jnp.max(scores, axis=-1, keepdims=True)
            if not diagonal:
                before = top[h][:, :1]
                peak = jnp.maximum(peak, before)
                fade = jnp.exp(before - peak)
            weights = jnp.exp(scores - peak)
            weight_sum = jnp.sum(weights, axis=-1, keepdims=True)
            part = dot(weights.astype(BF16), values[:, h * VDIM : (h + 1) * VDIM])
            if not diagonal:
                weight_sum = total[h][:, :1] * fade + weight_sum
                part = acc[h] * fade + part
            top[h] = jnp.broadcast_to(peak, (rows, LANES))
            total[h] = jnp.broadcast_to(weight_sum, (rows, LANES))
            acc[h] = part

    def window():
        @pl.when(sp > 0)
        def _():
            remote(tail, halo, halo_sem.at[0], halo_sem.at[1],
                   {"sp": sp, "tp": sibling}).wait_recv()

        @pl.when(sp == 0)
        def _():
            halo[...] = jnp.zeros(halo.shape, BF16)

        row = lax.broadcasted_iota(jnp.int32, (WINDOW, 2 * WINDOW), 0)
        column = lax.broadcasted_iota(jnp.int32, (WINDOW, 2 * WINDOW), 1)
        offset = row + WINDOW - column
        in_band = (offset >= 0) & (offset < WINDOW)
        for n in range(rows // WINDOW):
            at = slice(n * WINDOW, (n + 1) * WINDOW)
            earlier = halo[...] if n == 0 else local_kv[(n - 1) * WINDOW : n * WINDOW]
            band = jnp.concatenate([earlier, local_kv[at]], axis=0)
            valid = in_band & (sp * rows + n * WINDOW + column - WINDOW >= 0)
            heads = []
            for g in range(kv_heads):
                key = band[:, g * HEAD : (g + 1) * HEAD]
                value = band[:, kv_width + g * HEAD : kv_width + (g + 1) * HEAD]
                for i in range(group):
                    q = g * group + i
                    scores = dot_t(queries[at, q * HEAD : (q + 1) * HEAD], key) * HEAD ** (-0.5)
                    scores = jnp.where(valid, scores, NEGATIVE)
                    sink = sinks[0, q]
                    peak = jnp.maximum(jnp.max(scores, axis=-1, keepdims=True), sink)
                    weights = jnp.exp(scores - peak)
                    bottom = jnp.sum(weights, axis=-1, keepdims=True) + jnp.exp(sink - peak)
                    heads.append(dot((weights / bottom).astype(BF16), value))
            win[tp, at, :] = jnp.concatenate(heads, axis=1).astype(BF16)

    def gate(b):
        name = WEIGHTS[10 + b]
        loads[name].wait()

        def step(i, _):
            at = pl.ds(pl.multiple_of(i * 256, LANES), 256)
            gates[b, :, at] = jax.nn.sigmoid(dot(normed[...], w[name][:, at]))
            return 0

        lax.fori_loop(0, block // 256, step, 0)

    def step(k, _):
        @pl.when((z >= k) & (k < n_z))
        def _():
            take_column(k)

        @pl.when(z >= k - 1)
        def _():
            take_rows(k - 1)

        @pl.when(k == 1)
        def _():
            attend(sp, True)
            window()
            start(gather(win, 1))

        @pl.when(k == 2)
        def _():
            gate(0)
            gate(1)

        @pl.when((k > 1) & (z >= k - 1))
        def _():
            c_copy(k - 1, 1 - core).wait_recv()
            attend(column_slot(k - 1), False)

        for d in range(1, n_x):
            @pl.when(z >= k - 1)
            def _():
                d_copy(k - 1, d, 1 - core).wait_recv()

            @pl.when((z >= k - 1) & ((k > 1) | (lax.rem(x + n_x - d, n_x) < x)))
            def _():
                attend(row_slot(k - 1, d), False)

        return 0

    lax.fori_loop(1, max(n_z, 2) + 1, step, 0)

    for h in range(lat_heads):
        lat[tp, :, h * VDIM : (h + 1) * VDIM] = (acc[h] / total[h][:, :1]).astype(BF16)
    start(gather(lat, 2))
    arrived(win, 1)
    for copy in column_local:
        copy.wait()
    for b in range(2):
        for d in range(1, n_tp):
            source = lax.rem(tp + n_tp - d, n_tp)
            ref = columns[b].at[source]
            remote(ref, ref, col_send.at[b, d], col_recv.at[b, d],
                   {"sp": sp, "tp": sibling}).wait_recv()
    window_branch = jnp.zeros((rows, block), F32)
    for j in range(n_tp):
        window_branch = window_branch + dot(win[j], columns[0][j])
    wide_gated = gates[0] * window_branch
    gates[0] = wide_gated
    arrived(lat, 2)
    latent_branch = jnp.zeros((rows, block), F32)
    for j in range(n_tp):
        latent_branch = latent_branch + dot(lat[j], columns[1][j])
    out[...] = (gates[0] + gates[1] * latent_branch).astype(BF16)

    for buf, which in ((feat, 0), (win, 1), (lat, 2)):
        sent(buf, which)
    for copy in column_sends:
        copy.wait_send()

    @pl.when(sp + 1 < n_sp)
    def _():
        halo_copy.wait_send()

    def drain(k, _):
        @pl.when(z >= k)
        def _():
            @pl.when(z + 1 < n_z)
            def _():
                z_copy(k).wait_send()

            for d in range(1, n_x):
                x_copy(k, d).wait_send()
                d_copy(k, d, core).wait_send()

            @pl.when(k > 0)
            def _():
                c_copy(k, core).wait_send()

        return 0

    lax.fori_loop(0, n_z, drain, 0)


def on_device(dims, features, norm_gain, w_query, w_key, w_value, head_sinks, w_query_latent,
              w_kv_latent, w_rope_key, query_latent_gain, kv_latent_gain, w_query_content,
              w_query_rotary, w_key_up, w_value_up, w_branch_window, w_branch_latent,
              w_gate_window, w_gate_latent):
    n_sp, n_tp, n_x = dims
    n_z, n_y = n_sp // n_x, n_tp // 2
    rows, block = features.shape
    width = norm_gain.shape[0]
    latent = w_kv_latent.shape[1]
    lat_heads = w_key_up.shape[1] // NOPE
    positions = lax.axis_index("sp") * rows + jnp.arange(rows, dtype=jnp.int32)
    half_width = ROPE // 2
    frequencies = THETA ** (-jnp.arange(half_width, dtype=F32) / half_width)
    angles = positions.astype(F32)[:, None] * frequencies
    cosine, sine = jnp.cos(angles), jnp.sin(angles)
    cosine = jnp.concatenate([cosine, cosine], axis=1)
    sine = jnp.concatenate([-sine, sine], axis=1)
    weights = (w_kv_latent, w_rope_key, w_key, w_value, w_query, w_query_latent, w_query_content,
               w_query_rotary, w_key_up, w_value_up, w_gate_window, w_gate_latent)
    branches = (w_branch_window, w_branch_latent)
    vmem = pl.BlockSpec(memory_space=pltpu.VMEM)
    hbm = pl.BlockSpec(memory_space=pl.ANY)
    dma = pltpu.SemaphoreType.DMA
    return pl.pallas_call(
        functools.partial(kernel, dims),
        out_shape=jax.ShapeDtypeStruct((rows, block), BF16),
        in_specs=[hbm, vmem, pl.BlockSpec(memory_space=pltpu.SMEM), vmem, vmem, vmem, vmem]
        + [hbm] * (len(weights) + 2),
        out_specs=vmem,
        scratch_shapes=[
            pltpu.VMEM((n_tp, rows, block), BF16),
            pltpu.VMEM((rows, width), BF16),
            pltpu.VMEM((rows, latent), F32),
            *[pltpu.VMEM(weight.shape, BF16) for weight in weights],
            *[pltpu.VMEM((n_tp, branch.shape[0], block), BF16) for branch in branches],
            pltpu.VMEM((n_sp, 2, rows // 2, latent + LANES), BF16),
            pltpu.VMEM((rows, 2 * w_key.shape[1]), BF16),
            pltpu.VMEM((WINDOW, 2 * w_key.shape[1]), BF16),
            pltpu.VMEM((rows, w_query.shape[1]), BF16),
            pltpu.VMEM((lat_heads, rows, NOPE + LANES), BF16),
            pltpu.VMEM((2, rows, block), F32),
            pltpu.VMEM((n_tp, rows, w_query.shape[1]), BF16),
            pltpu.VMEM((n_tp, rows, lat_heads * VDIM), BF16),
            *[pltpu.VMEM((lat_heads, rows, LANES), F32)] * 3,
            dma((len(weights),)),
            dma((1,)),
            dma((2,)),
            dma((2, n_tp)),
            dma((2, n_tp)),
            dma((2,)),
            *[dma((3, n_y))] * 4,
            dma((n_z + 1,)),
            dma((n_z + 1,)),
            dma((n_z, n_x)),
            dma((n_z, n_x)),
            dma((n_z,)),
            dma((n_z,)),
            dma((n_z, n_x)),
            dma((n_z, n_x)),
        ],
        compiler_params=pltpu.CompilerParams(
            collective_id=0, has_side_effects=True, vmem_limit_bytes=60 * 1024 * 1024
        ),
    )(features, norm_gain[None, :], head_sinks[None, :], query_latent_gain[None, :],
      kv_latent_gain[None, :], cosine, sine, *weights, *branches)


def solution(mesh):
    n_sp, n_tp = mesh.shape["sp"], mesh.shape["tp"]
    n_x = 1
    while n_sp % (2 * n_x) == 0 and 8 * n_x * n_x <= n_sp:
        n_x *= 2
    return jax.shard_map(
        functools.partial(on_device, (n_sp, n_tp, n_x)),
        mesh=mesh,
        in_specs=(
            P("sp", "tp"),
            P(),
            P(None, "tp"),
            P(None, "tp"),
            P(None, "tp"),
            P("tp"),
            P(),
            P(),
            P(),
            P(),
            P(),
            P(None, "tp"),
            P(None, "tp"),
            P(None, "tp"),
            P(None, "tp"),
            P("tp", None),
            P("tp", None),
            P(None, "tp"),
            P(None, "tp"),
        ),
        out_specs=P("sp", "tp"),
        check_vma=False,
    )
```

```python
import functools

import jax
import jax.numpy as jnp
from jax import lax
from jax.experimental import pallas as pl
from jax.experimental.pallas import tpu as pltpu
from jax.sharding import PartitionSpec as P

HEAD = 64
WINDOW = 128
NOPE = 128
ROPE = 64
VDIM = 128


EPS = 1e-06
THETA = 10000.0
NEGATIVE = -1e30
LANES = 128
MESH = pl.DeviceIdType.MESH
BF16 = jnp.bfloat16
F32 = jnp.float32


def dot(left, right):
    return jnp.dot(left, right, preferred_element_type=F32)


def dot_t(left, right):
    return lax.dot_general(left, right, (((1,), (1,)), ((), ())), preferred_element_type=F32)


def rms_rows(rows, gain):
    return rows * lax.rsqrt(jnp.mean(rows * rows, axis=-1, keepdims=True) + EPS) * gain


def swap_halves(rows):
    half = rows.shape[1] // 2
    return jnp.concatenate([rows[:, half:], rows[:, :half]], axis=1)


WEIGHTS = (
    "kv_latent", "rope", "key", "value", "query", "query_latent", "content", "rotary",
    "key_up", "value_up", "gate_window", "gate_latent",
)


def kernel(dims, *refs):
    n_sp, n_tp, n_x = dims
    n_z, n_y = n_sp // n_x, n_tp // 2
    features, norm_gain, sinks, q_gain, kv_gain, frequency = refs[:6]
    refs = (None,) + refs
    w_hbm = dict(zip(WEIGHTS, refs[7:19]))
    branch_hbm = refs[19:21]
    out = refs[21]
    feat, normed, wide = refs[22:25]
    w = dict(zip(WEIGHTS, refs[25:37]))
    columns = refs[37:39]
    kvb, local_kv, halo, queries, q_full, gates, win, lat, top, total, acc = refs[39:50]
    w_sem, own_sem, col_own, col_send, col_recv, halo_sem, y_send, y_recv, s_send, s_recv = refs[50:60]
    z_send, z_recv, x_send, x_recv, c_send, c_recv, d_send, d_recv = refs[60:68]
    cosine, sine = refs[68:70]

    sp, tp = lax.axis_index("sp"), lax.axis_index("tp")
    z, x = sp // n_x, lax.rem(sp, n_x)
    y, core = tp // 2, lax.rem(tp, 2)
    sibling = y * 2 + (1 - core)
    rows, block = features.shape
    half = rows // 2
    lat_heads = w_hbm["key_up"].shape[1] // NOPE
    kv_width = w_hbm["key"].shape[1]
    kv_heads = kv_width // HEAD
    group = w_hbm["query"].shape[1] // kv_width
    latent = w_hbm["kv_latent"].shape[1]

    loads = {}
    own_feat = [
        pltpu.make_async_copy(features.at[pl.ds(h * half, half)], feat.at[tp, h], own_sem.at[h])
        for h in range(2)
    ]
    for copy in own_feat:
        copy.start()
    for i, name in enumerate(WEIGHTS):
        loads[name] = pltpu.make_async_copy(w_hbm[name], w[name], w_sem.at[i])
        loads[name].start()

    def remote(src, dst, send, recv, where):
        return pltpu.make_async_remote_copy(
            src_ref=src, dst_ref=dst, send_sem=send, recv_sem=recv,
            device_id=where, device_id_type=MESH,
        )

    barrier = pltpu.get_barrier_semaphore()

    def greet(where):
        pl.semaphore_signal(barrier, inc=1, device_id=where, device_id_type=MESH)

    for d in range(1, n_tp):
        greet({"sp": sp, "tp": lax.rem(tp + d, n_tp)})
    for d in range(1, n_x):
        greet({"sp": z * n_x + lax.rem(x + d, n_x), "tp": tp})

    @pl.when(z + 1 < n_z)
    def _():
        greet({"sp": sp + n_x, "tp": tp})

    @pl.when(z > 0)
    def _():
        greet({"sp": sp - n_x, "tp": tp})

    @pl.when(sp + 1 < n_sp)
    def _():
        greet({"sp": sp + 1, "tp": tp})

    @pl.when(sp > 0)
    def _():
        greet({"sp": sp - 1, "tp": tp})

    one, none = jnp.int32(1), jnp.int32(0)
    pl.semaphore_wait(
        barrier,
        n_tp - 1 + n_x - 1
        + jnp.where(z + 1 < n_z, one, none) + jnp.where(z > 0, one, none)
        + jnp.where(sp + 1 < n_sp, one, none) + jnp.where(sp > 0, one, none),
    )

    def gather(view, which):
        own = view(tp)
        sends = [
            remote(own, own, y_send.at[which, d], y_recv.at[which, d],
                   {"sp": sp, "tp": lax.rem(y + d, n_y) * 2 + core})
            for d in range(1, n_y)
        ]
        sends.append(remote(own, own, s_send.at[which, 0], s_recv.at[which, 0],
                            {"sp": sp, "tp": sibling}))
        return sends

    def start(copies):
        for copy in copies:
            copy.start()

    def forward(view, which):
        for d in range(1, n_y):
            ref = view(lax.rem(y + n_y - d, n_y) * 2 + core)
            remote(ref, ref, y_send.at[which, d], y_recv.at[which, d],
                   {"sp": sp, "tp": sibling}).wait_recv()
            remote(ref, ref, s_send.at[which, d], s_recv.at[which, d],
                   {"sp": sp, "tp": sibling}).start()

    def arrived(view, which):
        for d in range(n_y):
            ref = view(lax.rem(y + n_y - d, n_y) * 2 + (1 - core))
            remote(ref, ref, s_send.at[which, d], s_recv.at[which, d],
                   {"sp": sp, "tp": sibling}).wait_recv()

    def sent(view, which):
        own = view(tp)
        for d in range(1, n_y):
            remote(own, own, y_send.at[which, d], y_recv.at[which, d],
                   {"sp": sp, "tp": sibling}).wait_send()
        for d in range(n_y):
            remote(own, own, s_send.at[which, d], s_recv.at[which, d],
                   {"sp": sp, "tp": sibling}).wait_send()

    feat_half = [lambda slot, h=h: feat.at[slot, h] for h in range(2)]
    lat_half = [lambda slot, h=h: lat.at[slot, h] for h in range(2)]
    win_all = lambda slot: win.at[slot]

    for h in range(2):
        own_feat[h].wait()
        start(gather(feat_half[h], h))

    positions = (sp * rows + lax.broadcasted_iota(jnp.int32, (rows, ROPE), 0)).astype(F32)
    angles = positions * frequency[...]
    lane = lax.broadcasted_iota(jnp.int32, (rows, ROPE), 1)
    cosine[...] = jnp.cos(angles)
    turned = jnp.sin(angles)
    sine[...] = jnp.where(lane < ROPE // 2, -turned, turned)

    def column_copies():
        local, sends = [], []
        for b in range(2):
            span = branch_hbm[b]
            local.append(pltpu.make_async_copy(
                span.at[:, pl.ds(pl.multiple_of(tp * block, LANES), block)],
                columns[b].at[tp], col_own.at[b]))
            for d in range(1, n_tp):
                to = lax.rem(tp + d, n_tp)
                sends.append(remote(
                    span.at[:, pl.ds(pl.multiple_of(to * block, LANES), block)],
                    columns[b].at[tp], col_send.at[b, d], col_recv.at[b, d],
                    {"sp": sp, "tp": to}))
        return local, sends

    column_local, column_sends = column_copies()

    def normalize(h):
        squares = jnp.zeros((half, 1), F32)
        for j in range(n_tp):
            piece = feat[j, h].astype(F32)
            squares = squares + jnp.sum(piece * piece, axis=-1, keepdims=True)
        scale = lax.rsqrt(squares / (n_tp * block) + EPS)
        for j in range(n_tp):
            span = slice(j * block, (j + 1) * block)
            piece = feat[j, h].astype(F32) * scale * norm_gain[:, span]
            normed[h * half : (h + 1) * half, span] = piece.astype(BF16)

    def wide_dot(name, at):
        tile = min(256, latent)

        def step(i, _):
            to = pl.ds(pl.multiple_of(i * tile, LANES), tile)
            wide[at, to] = dot(normed[at, :], w[name][:, to])
            return 0

        lax.fori_loop(0, w[name].shape[1] // tile, step, 0)

    padding = jnp.zeros((rows, LANES - ROPE), F32)

    def latents(h):
        at = slice(h * half, (h + 1) * half)
        wide_dot("kv_latent", at)
        rope = dot_t(normed[at, :], w["rope"][...])
        rope = rope * cosine[at, :] + swap_halves(rope) * sine[at, :]
        rope = jnp.concatenate([rope, padding[at]], axis=1).astype(BF16)
        kvb[sp, h, :, :, :latent] = (
            rms_rows(wide[at, :], kv_gain[...]).astype(BF16).reshape(2, half // 2, latent))
        kvb[sp, h, :, :, latent:] = rope.reshape(2, half // 2, LANES)

    def column_slot(k):
        return (z - k) * n_x + x

    def row_slot(k, d):
        return (z - k) * n_x + lax.rem(x + n_x - d, n_x)

    def z_copy(k, h):
        ref = kvb.at[column_slot(k), h, core]
        return remote(ref, ref, z_send.at[h, k], z_recv.at[h, k + 1], {"sp": sp + n_x, "tp": tp})

    def x_copy(k, d, h):
        ref = kvb.at[column_slot(k), h, core]
        return remote(ref, ref, x_send.at[h, k, d], x_recv.at[h, k, d],
                      {"sp": z * n_x + lax.rem(x + d, n_x), "tp": tp})

    def c_copy(k, h, which):
        ref = kvb.at[column_slot(k), h, which]
        return remote(ref, ref, c_send.at[h, k], c_recv.at[h, k], {"sp": sp, "tp": sibling})

    def d_copy(k, d, h, which):
        ref = kvb.at[row_slot(k, d), h, which]
        return remote(ref, ref, d_send.at[h, k, d], d_recv.at[h, k, d],
                      {"sp": sp, "tp": sibling})

    def pass_on(k, h):
        @pl.when(z + 1 < n_z)
        def _():
            z_copy(k, h).start()

        for d in range(1, n_x):
            x_copy(k, d, h).start()

    def take_column(k):
        for h in range(2):
            ref = kvb.at[column_slot(k), h, core]
            remote(ref, ref, z_send.at[h, k], z_recv.at[h, k],
                   {"sp": sp, "tp": sibling}).wait_recv()
            pass_on(k, h)
            c_copy(k, h, core).start()

    def take_rows(k):
        for h in range(2):
            for d in range(1, n_x):
                ref = kvb.at[row_slot(k, d), h, core]
                remote(ref, ref, x_send.at[h, k, d], x_recv.at[h, k, d],
                       {"sp": sp, "tp": sibling}).wait_recv()
                d_copy(k, d, h, core).start()

    loads["kv_latent"].wait()
    loads["rope"].wait()
    for h in range(2):
        forward(feat_half[h], h)
        arrived(feat_half[h], h)
        if h == 1:
            start(column_local)
            start(column_sends)
        normalize(h)
        latents(h)
        pass_on(0, h)

    loads["key"].wait()
    loads["value"].wait()
    local_kv[:, :kv_width] = dot(normed[...], w["key"][...]).astype(BF16)
    local_kv[:, kv_width:] = dot(normed[...], w["value"][...]).astype(BF16)
    tail = local_kv.at[pl.ds(rows - WINDOW, WINDOW)]
    halo_copy = remote(tail, halo, halo_sem.at[0], halo_sem.at[1], {"sp": sp + 1, "tp": tp})

    @pl.when(sp + 1 < n_sp)
    def _():
        halo_copy.start()

    loads["query"].wait()
    queries[...] = dot(normed[...], w["query"][...]).astype(BF16)

    loads["query_latent"].wait()
    wide_dot("query_latent", slice(0, rows))
    latent_query = rms_rows(wide[...], q_gain[...]).astype(BF16)
    loads["content"].wait()
    loads["rotary"].wait()
    content = dot(latent_query, w["content"][...]).astype(BF16)
    rotary = dot(latent_query, w["rotary"][...])
    for h in range(lat_heads):
        turned = rotary[:, h * ROPE : (h + 1) * ROPE]
        turned = turned * cosine[...] + swap_halves(turned) * sine[...]
        q_full[h, :, :NOPE] = content[:, h * NOPE : (h + 1) * NOPE]
        q_full[h, :, NOPE:] = jnp.concatenate([turned, padding], axis=1).astype(BF16)
    loads["key_up"].wait()
    loads["value_up"].wait()

    def attend(slot, diagonal):
        both = kvb[slot].reshape(rows, latent + LANES)
        source, rope_part = both[:, :latent], both[:, latent:]
        keys = dot(source, w["key_up"][...]).astype(BF16)
        values = dot(source, w["value_up"][...]).astype(BF16)
        for h in range(lat_heads):
            key = jnp.concatenate([keys[:, h * NOPE : (h + 1) * NOPE], rope_part], axis=1)
            scores = dot_t(q_full[h], key) * (NOPE + ROPE) ** (-0.5)
            if diagonal:
                live = (lax.broadcasted_iota(jnp.int32, scores.shape, 1)
                        <= lax.broadcasted_iota(jnp.int32, scores.shape, 0))
                scores = jnp.where(live, scores, NEGATIVE)
            peak = jnp.max(scores, axis=-1, keepdims=True)
            if not diagonal:
                before = top[h][:, :1]
                peak = jnp.maximum(peak, before)
                fade = jnp.exp(before - peak)
            weights = jnp.exp(scores - peak)
            weight_sum = jnp.sum(weights, axis=-1, keepdims=True)
            part = dot(weights.astype(BF16), values[:, h * VDIM : (h + 1) * VDIM])
            if not diagonal:
                weight_sum = total[h][:, :1] * fade + weight_sum
                part = acc[h] * fade + part
            top[h] = jnp.broadcast_to(peak, (rows, LANES))
            total[h] = jnp.broadcast_to(weight_sum, (rows, LANES))
            acc[h] = part

    def window():
        @pl.when(sp > 0)
        def _():
            remote(tail, halo, halo_sem.at[0], halo_sem.at[1],
                   {"sp": sp, "tp": sibling}).wait_recv()

        @pl.when(sp == 0)
        def _():
            halo[...] = jnp.zeros(halo.shape, BF16)

        row = lax.broadcasted_iota(jnp.int32, (WINDOW, 2 * WINDOW), 0)
        column = lax.broadcasted_iota(jnp.int32, (WINDOW, 2 * WINDOW), 1)
        offset = row + WINDOW - column
        in_band = (offset >= 0) & (offset < WINDOW)
        for n in range(rows // WINDOW):
            at = slice(n * WINDOW, (n + 1) * WINDOW)
            earlier = halo[...] if n == 0 else local_kv[(n - 1) * WINDOW : n * WINDOW]
            band = jnp.concatenate([earlier, local_kv[at]], axis=0)
            valid = in_band & (sp * rows + n * WINDOW + column - WINDOW >= 0)
            heads = []
            for g in range(kv_heads):
                key = band[:, g * HEAD : (g + 1) * HEAD]
                value = band[:, kv_width + g * HEAD : kv_width + (g + 1) * HEAD]
                for i in range(group):
                    q = g * group + i
                    scores = dot_t(queries[at, q * HEAD : (q + 1) * HEAD], key) * HEAD ** (-0.5)
                    scores = jnp.where(valid, scores, NEGATIVE)
                    sink = sinks[0, q]
                    peak = jnp.maximum(jnp.max(scores, axis=-1, keepdims=True), sink)
                    weights = jnp.exp(scores - peak)
                    bottom = jnp.sum(weights, axis=-1, keepdims=True) + jnp.exp(sink - peak)
                    heads.append(dot((weights / bottom).astype(BF16), value))
            win[tp, at, :] = jnp.concatenate(heads, axis=1).astype(BF16)

    def gate(b):
        name = WEIGHTS[10 + b]
        loads[name].wait()

        def step(i, _):
            at = pl.ds(pl.multiple_of(i * 256, LANES), 256)
            gates[b, :, at] = jax.nn.sigmoid(dot(normed[...], w[name][:, at]))
            return 0

        lax.fori_loop(0, block // 256, step, 0)

    def step(k, _):
        @pl.when((z >= k) & (k < n_z))
        def _():
            take_column(k)

        @pl.when(k == 1)
        def _():
            attend(sp, True)

        @pl.when(k == 2)
        def _():
            window()
            start(gather(win_all, 2))

        @pl.when(k == 3)
        def _():
            gate(0)
            gate(1)

        @pl.when((k > 1) & (z >= k - 1))
        def _():
            for h in range(2):
                c_copy(k - 1, h, 1 - core).wait_recv()
            attend(column_slot(k - 1), False)

        @pl.when(z >= k - 1)
        def _():
            take_rows(k - 1)

        for d in range(1, n_x):
            @pl.when(z >= k - 1)
            def _():
                for h in range(2):
                    d_copy(k - 1, d, h, 1 - core).wait_recv()

            @pl.when((z >= k - 1) & ((k > 1) | (lax.rem(x + n_x - d, n_x) < x)))
            def _():
                attend(row_slot(k - 1, d), False)

        return 0

    lax.fori_loop(1, max(n_z, 3) + 1, step, 0)

    for part in range(2):
        at = slice(part * half, (part + 1) * half)
        for h in range(lat_heads):
            lat[tp, part, :, h * VDIM : (h + 1) * VDIM] = (
                acc[h, at] / total[h, at][:, :1]).astype(BF16)
        start(gather(lat_half[part], 3 + part))
    forward(win_all, 2)
    arrived(win_all, 2)
    for copy in column_local:
        copy.wait()
    for b in range(2):
        for d in range(1, n_tp):
            source = lax.rem(tp + n_tp - d, n_tp)
            ref = columns[b].at[source]
            remote(ref, ref, col_send.at[b, d], col_recv.at[b, d],
                   {"sp": sp, "tp": sibling}).wait_recv()
    window_branch = jnp.zeros((rows, block), F32)
    for j in range(n_tp):
        window_branch = window_branch + dot(win[j], columns[0][j])
    gates[0] = gates[0] * window_branch
    for part in range(2):
        at = slice(part * half, (part + 1) * half)
        forward(lat_half[part], 3 + part)
        arrived(lat_half[part], 3 + part)
        latent_branch = jnp.zeros((half, block), F32)
        for j in range(n_tp):
            latent_branch = latent_branch + dot(lat[j, part], columns[1][j])
        out[at, :] = (gates[0, at] + gates[1, at] * latent_branch).astype(BF16)

    for which, view in enumerate((*feat_half, win_all, *lat_half)):
        sent(view, which)
    for copy in column_sends:
        copy.wait_send()

    @pl.when(sp + 1 < n_sp)
    def _():
        halo_copy.wait_send()

    def drain(k, _):
        @pl.when(z >= k)
        def _():
            for h in range(2):
                @pl.when(z + 1 < n_z)
                def _():
                    z_copy(k, h).wait_send()

                for d in range(1, n_x):
                    x_copy(k, d, h).wait_send()
                    d_copy(k, d, h, core).wait_send()

                @pl.when(k > 0)
                def _():
                    c_copy(k, h, core).wait_send()

        return 0

    lax.fori_loop(0, n_z, drain, 0)


def on_device(dims, features, norm_gain, w_query, w_key, w_value, head_sinks, w_query_latent,
              w_kv_latent, w_rope_key, query_latent_gain, kv_latent_gain, w_query_content,
              w_query_rotary, w_key_up, w_value_up, w_branch_window, w_branch_latent,
              w_gate_window, w_gate_latent):
    n_sp, n_tp, n_x = dims
    n_z, n_y = n_sp // n_x, n_tp // 2
    rows, block = features.shape
    width = norm_gain.shape[0]
    latent = w_kv_latent.shape[1]
    lat_heads = w_key_up.shape[1] // NOPE
    half_width = ROPE // 2
    entry = lax.rem(jnp.arange(ROPE, dtype=jnp.int32), half_width).astype(F32)
    frequency = (THETA ** (-entry / half_width))[None, :]
    weights = (w_kv_latent, w_rope_key.T, w_key, w_value, w_query, w_query_latent, w_query_content,
               w_query_rotary, w_key_up, w_value_up, w_gate_window, w_gate_latent)
    branches = (w_branch_window, w_branch_latent)
    vmem = pl.BlockSpec(memory_space=pltpu.VMEM)
    hbm = pl.BlockSpec(memory_space=pl.ANY)
    dma = pltpu.SemaphoreType.DMA
    return pl.pallas_call(
        functools.partial(kernel, dims),
        out_shape=jax.ShapeDtypeStruct((rows, block), BF16),
        in_specs=[hbm, vmem, pl.BlockSpec(memory_space=pltpu.SMEM), vmem, vmem, vmem]
        + [hbm] * (len(weights) + 2),
        out_specs=vmem,
        scratch_shapes=[
            pltpu.VMEM((n_tp, 2, rows // 2, block), BF16),
            pltpu.VMEM((rows, width), BF16),
            pltpu.VMEM((rows, latent), F32),
            *[pltpu.VMEM(weight.shape, BF16) for weight in weights],
            *[pltpu.VMEM((n_tp, branch.shape[0], block), BF16) for branch in branches],
            pltpu.VMEM((n_sp, 2, 2, rows // 4, latent + LANES), BF16),
            pltpu.VMEM((rows, 2 * w_key.shape[1]), BF16),
            pltpu.VMEM((WINDOW, 2 * w_key.shape[1]), BF16),
            pltpu.VMEM((rows, w_query.shape[1]), BF16),
            pltpu.VMEM((lat_heads, rows, NOPE + LANES), BF16),
            pltpu.VMEM((2, rows, block), F32),
            pltpu.VMEM((n_tp, rows, w_query.shape[1]), BF16),
            pltpu.VMEM((n_tp, 2, rows // 2, lat_heads * VDIM), BF16),
            *[pltpu.VMEM((lat_heads, rows, LANES), F32)] * 3,
            dma((len(weights),)),
            dma((2,)),
            dma((2,)),
            dma((2, n_tp)),
            dma((2, n_tp)),
            dma((2,)),
            *[dma((5, n_y))] * 4,
            dma((2, n_z + 1)),
            dma((2, n_z + 1)),
            dma((2, n_z, n_x)),
            dma((2, n_z, n_x)),
            dma((2, n_z)),
            dma((2, n_z)),
            dma((2, n_z, n_x)),
            dma((2, n_z, n_x)),
            *[pltpu.VMEM((rows, ROPE), F32)] * 2,
        ],
        compiler_params=pltpu.CompilerParams(
            collective_id=0, has_side_effects=True, vmem_limit_bytes=60 * 1024 * 1024
        ),
    )(features, norm_gain[None, :], head_sinks[None, :], query_latent_gain[None, :],
      kv_latent_gain[None, :], frequency, *weights, *branches)


def solution(mesh):
    n_sp, n_tp = mesh.shape["sp"], mesh.shape["tp"]
    n_x = 1
    while n_sp % (2 * n_x) == 0 and 8 * n_x * n_x <= n_sp:
        n_x *= 2
    return jax.shard_map(
        functools.partial(on_device, (n_sp, n_tp, n_x)),
        mesh=mesh,
        in_specs=(
            P("sp", "tp"),
            P(),
            P(None, "tp"),
            P(None, "tp"),
            P(None, "tp"),
            P("tp"),
            P(),
            P(),
            P(),
            P(),
            P(),
            P(None, "tp"),
            P(None, "tp"),
            P(None, "tp"),
            P(None, "tp"),
            P("tp", None),
            P("tp", None),
            P(None, "tp"),
            P(None, "tp"),
        ),
        out_specs=P("sp", "tp"),
        check_vma=False,
    )
```

```python
import functools

import jax
import jax.numpy as jnp
from jax import lax
from jax.experimental import pallas as pl
from jax.experimental.pallas import tpu as pltpu
from jax.sharding import PartitionSpec as P

HEAD = 64
WINDOW = 128
NOPE = 128
ROPE = 64
VDIM = 128


EPS = 1e-06
THETA = 10000.0
NEGATIVE = -1e30
LANES = 128
LOG2_E = 1.4426950408889634
MESH = pl.DeviceIdType.MESH
BF16 = jnp.bfloat16
F32 = jnp.float32


def dot(left, right):
    return jnp.dot(left, right, preferred_element_type=F32)


def dot_t(left, right):
    return lax.dot_general(left, right, (((1,), (1,)), ((), ())), preferred_element_type=F32)


def rms_rows(rows, gain):
    return rows * lax.rsqrt(jnp.mean(rows * rows, axis=-1, keepdims=True) + EPS) * gain


def swap_halves(rows):
    half = rows.shape[1] // 2
    return jnp.concatenate([rows[:, half:], rows[:, :half]], axis=1)


WEIGHTS = (
    "kv_latent", "rope", "key", "value", "query", "query_latent", "content", "rotary",
    "key_up", "value_up", "gate_window", "gate_latent",
)


def kernel(dims, *refs):
    n_sp, n_tp, n_x = dims
    n_z, n_y = n_sp // n_x, n_tp // 2
    features, norm_gain, sinks, q_gain, kv_gain, frequency = refs[:6]
    refs = (None,) + refs
    w_hbm = dict(zip(WEIGHTS, refs[7:19]))
    branch_hbm = refs[19:21]
    out = refs[21]
    feat, normed, wide = refs[22:25]
    w = dict(zip(WEIGHTS, refs[25:37]))
    columns = refs[37:39]
    kvb, local_kv, halo, queries, q_full, gates, win, lat, top, total, acc = refs[39:50]
    w_sem, own_sem, col_own, col_send, col_recv, halo_sem, y_send, y_recv, s_send, s_recv = refs[50:60]
    z_send, z_recv, x_send, x_recv, c_send, c_recv, d_send, d_recv = refs[60:68]
    cosine, sine = refs[68:70]

    sp, tp = lax.axis_index("sp"), lax.axis_index("tp")
    z, x = sp // n_x, lax.rem(sp, n_x)
    y, core = tp // 2, lax.rem(tp, 2)
    sibling = y * 2 + (1 - core)
    rows, block = features.shape
    half = rows // 2
    lat_heads = w_hbm["key_up"].shape[1] // NOPE
    kv_width = w_hbm["key"].shape[1]
    kv_heads = kv_width // HEAD
    group = w_hbm["query"].shape[1] // kv_width
    latent = w_hbm["kv_latent"].shape[1]

    loads = {}
    own_feat = [
        pltpu.make_async_copy(features.at[pl.ds(h * half, half)], feat.at[tp, h], own_sem.at[h])
        for h in range(2)
    ]
    for copy in own_feat:
        copy.start()
    for i, name in enumerate(WEIGHTS):
        loads[name] = pltpu.make_async_copy(w_hbm[name], w[name], w_sem.at[i])
        loads[name].start()

    def remote(src, dst, send, recv, where):
        return pltpu.make_async_remote_copy(
            src_ref=src, dst_ref=dst, send_sem=send, recv_sem=recv,
            device_id=where, device_id_type=MESH,
        )

    barrier = pltpu.get_barrier_semaphore()

    def greet(where):
        pl.semaphore_signal(barrier, inc=1, device_id=where, device_id_type=MESH)

    for d in range(1, n_tp):
        greet({"sp": sp, "tp": lax.rem(tp + d, n_tp)})
    for d in range(1, n_x):
        greet({"sp": z * n_x + lax.rem(x + d, n_x), "tp": tp})

    @pl.when(z + 1 < n_z)
    def _():
        greet({"sp": sp + n_x, "tp": tp})

    @pl.when(z > 0)
    def _():
        greet({"sp": sp - n_x, "tp": tp})

    @pl.when(sp + 1 < n_sp)
    def _():
        greet({"sp": sp + 1, "tp": tp})

    @pl.when(sp > 0)
    def _():
        greet({"sp": sp - 1, "tp": tp})

    one, none = jnp.int32(1), jnp.int32(0)
    pl.semaphore_wait(
        barrier,
        n_tp - 1 + n_x - 1
        + jnp.where(z + 1 < n_z, one, none) + jnp.where(z > 0, one, none)
        + jnp.where(sp + 1 < n_sp, one, none) + jnp.where(sp > 0, one, none),
    )

    def gather(view, which):
        own = view(tp)
        sends = [
            remote(own, own, y_send.at[which, d], y_recv.at[which, d],
                   {"sp": sp, "tp": lax.rem(y + d, n_y) * 2 + core})
            for d in range(1, n_y)
        ]
        sends.append(remote(own, own, s_send.at[which, 0], s_recv.at[which, 0],
                            {"sp": sp, "tp": sibling}))
        return sends

    def start(copies):
        for copy in copies:
            copy.start()

    def forward(view, which):
        for d in range(1, n_y):
            ref = view(lax.rem(y + n_y - d, n_y) * 2 + core)
            remote(ref, ref, y_send.at[which, d], y_recv.at[which, d],
                   {"sp": sp, "tp": sibling}).wait_recv()
            remote(ref, ref, s_send.at[which, d], s_recv.at[which, d],
                   {"sp": sp, "tp": sibling}).start()

    def arrived(view, which):
        for d in range(n_y):
            ref = view(lax.rem(y + n_y - d, n_y) * 2 + (1 - core))
            remote(ref, ref, s_send.at[which, d], s_recv.at[which, d],
                   {"sp": sp, "tp": sibling}).wait_recv()

    def sent(view, which):
        own = view(tp)
        for d in range(1, n_y):
            remote(own, own, y_send.at[which, d], y_recv.at[which, d],
                   {"sp": sp, "tp": sibling}).wait_send()
        for d in range(n_y):
            remote(own, own, s_send.at[which, d], s_recv.at[which, d],
                   {"sp": sp, "tp": sibling}).wait_send()

    feat_half = [lambda slot, h=h: feat.at[slot, h] for h in range(2)]
    lat_half = [lambda slot, h=h: lat.at[slot, h] for h in range(2)]
    win_all = lambda slot: win.at[slot]

    for h in range(2):
        own_feat[h].wait()
        start(gather(feat_half[h], h))

    positions = (sp * rows + lax.broadcasted_iota(jnp.int32, (rows, ROPE), 0)).astype(F32)
    angles = positions * frequency[...]
    lane = lax.broadcasted_iota(jnp.int32, (rows, ROPE), 1)
    cosine[...] = jnp.cos(angles)
    turned = jnp.sin(angles)
    sine[...] = jnp.where(lane < ROPE // 2, -turned, turned)

    def column_copies():
        local, sends = [], []
        for b in range(2):
            span = branch_hbm[b]
            local.append(pltpu.make_async_copy(
                span.at[:, pl.ds(pl.multiple_of(tp * block, LANES), block)],
                columns[b].at[tp], col_own.at[b]))
            for d in range(1, n_tp):
                to = lax.rem(tp + d, n_tp)
                sends.append(remote(
                    span.at[:, pl.ds(pl.multiple_of(to * block, LANES), block)],
                    columns[b].at[tp], col_send.at[b, d], col_recv.at[b, d],
                    {"sp": sp, "tp": to}))
        return local, sends

    column_local, column_sends = column_copies()

    def normalize(h):
        squares = jnp.zeros((half, 1), F32)
        for j in range(n_tp):
            piece = feat[j, h].astype(F32)
            squares = squares + jnp.sum(piece * piece, axis=-1, keepdims=True)
        scale = lax.rsqrt(squares / (n_tp * block) + EPS)
        for j in range(n_tp):
            span = slice(j * block, (j + 1) * block)
            piece = feat[j, h].astype(F32) * scale * norm_gain[:, span]
            normed[h * half : (h + 1) * half, span] = piece.astype(BF16)

    def wide_dot(name, at):
        tile = min(256, latent)

        def step(i, _):
            to = pl.ds(pl.multiple_of(i * tile, LANES), tile)
            wide[at, to] = dot(normed[at, :], w[name][:, to])
            return 0

        lax.fori_loop(0, w[name].shape[1] // tile, step, 0)

    padding = jnp.zeros((rows, LANES - ROPE), F32)

    def latents(h):
        at = slice(h * half, (h + 1) * half)
        wide_dot("kv_latent", at)
        rope = dot_t(normed[at, :], w["rope"][...])
        rope = rope * cosine[at, :] + swap_halves(rope) * sine[at, :]
        rope = jnp.concatenate([rope, padding[at]], axis=1).astype(BF16)
        kvb[sp, h, :, :, :latent] = (
            rms_rows(wide[at, :], kv_gain[...]).astype(BF16).reshape(2, half // 2, latent))
        kvb[sp, h, :, :, latent:] = rope.reshape(2, half // 2, LANES)

    def column_slot(k):
        return (z - k) * n_x + x

    def row_slot(k, d):
        return (z - k) * n_x + lax.rem(x + n_x - d, n_x)

    def z_copy(k, h):
        ref = kvb.at[column_slot(k), h, core]
        return remote(ref, ref, z_send.at[h, k], z_recv.at[h, k + 1], {"sp": sp + n_x, "tp": tp})

    def x_copy(k, d, h):
        ref = kvb.at[column_slot(k), h, core]
        return remote(ref, ref, x_send.at[h, k, d], x_recv.at[h, k, d],
                      {"sp": z * n_x + lax.rem(x + d, n_x), "tp": tp})

    def c_copy(k, h, which):
        ref = kvb.at[column_slot(k), h, which]
        return remote(ref, ref, c_send.at[h, k], c_recv.at[h, k], {"sp": sp, "tp": sibling})

    def d_copy(k, d, h, which):
        ref = kvb.at[row_slot(k, d), h, which]
        return remote(ref, ref, d_send.at[h, k, d], d_recv.at[h, k, d],
                      {"sp": sp, "tp": sibling})

    def pass_on(k, h):
        @pl.when(z + 1 < n_z)
        def _():
            z_copy(k, h).start()

        for d in range(1, n_x):
            x_copy(k, d, h).start()

    def take_column(k):
        for h in range(2):
            ref = kvb.at[column_slot(k), h, core]
            remote(ref, ref, z_send.at[h, k], z_recv.at[h, k],
                   {"sp": sp, "tp": sibling}).wait_recv()
            pass_on(k, h)
            c_copy(k, h, core).start()

    def take_rows(k):
        for h in range(2):
            for d in range(1, n_x):
                ref = kvb.at[row_slot(k, d), h, core]
                remote(ref, ref, x_send.at[h, k, d], x_recv.at[h, k, d],
                       {"sp": sp, "tp": sibling}).wait_recv()
                d_copy(k, d, h, core).start()

    loads["kv_latent"].wait()
    loads["rope"].wait()
    for h in range(2):
        forward(feat_half[h], h)
        arrived(feat_half[h], h)
        if h == 1:
            start(column_local)
            start(column_sends)
        normalize(h)
        latents(h)
        pass_on(0, h)

    loads["key"].wait()
    loads["value"].wait()
    local_kv[:, :kv_width] = dot(normed[...], w["key"][...]).astype(BF16)
    local_kv[:, kv_width:] = dot(normed[...], w["value"][...]).astype(BF16)
    tail = local_kv.at[pl.ds(rows - WINDOW, WINDOW)]
    halo_copy = remote(tail, halo, halo_sem.at[0], halo_sem.at[1], {"sp": sp + 1, "tp": tp})

    @pl.when(sp + 1 < n_sp)
    def _():
        halo_copy.start()

    loads["query"].wait()
    queries[...] = dot(normed[...], w["query"][...]).astype(BF16)

    loads["query_latent"].wait()
    wide_dot("query_latent", slice(0, rows))
    latent_query = rms_rows(wide[...], q_gain[...]).astype(BF16)
    loads["content"].wait()
    loads["rotary"].wait()
    content = dot(latent_query, w["content"][...]).astype(BF16)
    rotary = dot(latent_query, w["rotary"][...])
    for h in range(lat_heads):
        turned = rotary[:, h * ROPE : (h + 1) * ROPE]
        turned = turned * cosine[...] + swap_halves(turned) * sine[...]
        q_full[h, :, :NOPE] = content[:, h * NOPE : (h + 1) * NOPE]
        q_full[h, :, NOPE:] = jnp.concatenate([turned, padding], axis=1).astype(BF16)
    loads["key_up"].wait()
    loads["value_up"].wait()

    def attend(slot, diagonal):
        both = kvb[slot].reshape(rows, latent + LANES)
        source, rope_part = both[:, :latent], both[:, latent:]
        keys = dot(source, w["key_up"][...]).astype(BF16)
        values = dot(source, w["value_up"][...]).astype(BF16)
        for h in range(lat_heads):
            key = jnp.concatenate([keys[:, h * NOPE : (h + 1) * NOPE], rope_part], axis=1)
            scores = dot_t(q_full[h], key) * ((NOPE + ROPE) ** (-0.5) * LOG2_E)
            if diagonal:
                live = (lax.broadcasted_iota(jnp.int32, scores.shape, 1)
                        <= lax.broadcasted_iota(jnp.int32, scores.shape, 0))
                scores = jnp.where(live, scores, NEGATIVE)
            peak = jnp.max(scores, axis=-1, keepdims=True)
            if not diagonal:
                before = top[h][:, :1]
                peak = jnp.maximum(peak, before)
                fade = jnp.exp2(before - peak)
            weights = jnp.exp2(scores - peak)
            weight_sum = jnp.sum(weights, axis=-1, keepdims=True)
            part = dot(weights.astype(BF16), values[:, h * VDIM : (h + 1) * VDIM])
            if not diagonal:
                weight_sum = total[h][:, :1] * fade + weight_sum
                part = acc[h] * fade + part
            top[h] = jnp.broadcast_to(peak, (rows, LANES))
            total[h] = jnp.broadcast_to(weight_sum, (rows, LANES))
            acc[h] = part

    def window():
        @pl.when(sp > 0)
        def _():
            remote(tail, halo, halo_sem.at[0], halo_sem.at[1],
                   {"sp": sp, "tp": sibling}).wait_recv()

        @pl.when(sp == 0)
        def _():
            halo[...] = jnp.zeros(halo.shape, BF16)

        row = lax.broadcasted_iota(jnp.int32, (WINDOW, 2 * WINDOW), 0)
        column = lax.broadcasted_iota(jnp.int32, (WINDOW, 2 * WINDOW), 1)
        offset = row + WINDOW - column
        in_band = (offset >= 0) & (offset < WINDOW)
        for n in range(rows // WINDOW):
            at = slice(n * WINDOW, (n + 1) * WINDOW)
            earlier = halo[...] if n == 0 else local_kv[(n - 1) * WINDOW : n * WINDOW]
            band = jnp.concatenate([earlier, local_kv[at]], axis=0)
            valid = in_band & (sp * rows + n * WINDOW + column - WINDOW >= 0)
            heads = []
            for g in range(kv_heads):
                key = band[:, g * HEAD : (g + 1) * HEAD]
                value = band[:, kv_width + g * HEAD : kv_width + (g + 1) * HEAD]
                for i in range(group):
                    q = g * group + i
                    scores = dot_t(queries[at, q * HEAD : (q + 1) * HEAD], key) * HEAD ** (-0.5)
                    scores = jnp.where(valid, scores, NEGATIVE)
                    sink = sinks[0, q]
                    peak = jnp.maximum(jnp.max(scores, axis=-1, keepdims=True), sink)
                    weights = jnp.exp(scores - peak)
                    bottom = jnp.sum(weights, axis=-1, keepdims=True) + jnp.exp(sink - peak)
                    heads.append(dot((weights / bottom).astype(BF16), value))
            win[tp, at, :] = jnp.concatenate(heads, axis=1).astype(BF16)

    def gate(b):
        name = WEIGHTS[10 + b]
        loads[name].wait()

        def step(i, _):
            at = pl.ds(pl.multiple_of(i * 256, LANES), 256)
            gates[b, :, at] = jax.nn.sigmoid(dot(normed[...], w[name][:, at]))
            return 0

        lax.fori_loop(0, block // 256, step, 0)

    def step(k, _):
        @pl.when((z >= k) & (k < n_z))
        def _():
            take_column(k)

        @pl.when(k == 1)
        def _():
            attend(sp, True)

        @pl.when(k == 2)
        def _():
            window()
            start(gather(win_all, 2))

        @pl.when((k > 1) & (z >= k - 1))
        def _():
            for h in range(2):
                c_copy(k - 1, h, 1 - core).wait_recv()
            attend(column_slot(k - 1), False)

        @pl.when(z >= k - 1)
        def _():
            take_rows(k - 1)

        for d in range(1, n_x):
            @pl.when(z >= k - 1)
            def _():
                for h in range(2):
                    d_copy(k - 1, d, h, 1 - core).wait_recv()

            @pl.when((z >= k - 1) & ((k > 1) | (lax.rem(x + n_x - d, n_x) < x)))
            def _():
                attend(row_slot(k - 1, d), False)

        return 0

    lax.fori_loop(1, max(n_z, 2) + 1, step, 0)

    for part in range(2):
        at = slice(part * half, (part + 1) * half)
        for h in range(lat_heads):
            lat[tp, part, :, h * VDIM : (h + 1) * VDIM] = (
                acc[h, at] / total[h, at][:, :1]).astype(BF16)
        start(gather(lat_half[part], 3 + part))
    gate(0)
    forward(win_all, 2)
    gate(1)
    arrived(win_all, 2)
    for copy in column_local:
        copy.wait()
    for b in range(2):
        for d in range(1, n_tp):
            source = lax.rem(tp + n_tp - d, n_tp)
            ref = columns[b].at[source]
            remote(ref, ref, col_send.at[b, d], col_recv.at[b, d],
                   {"sp": sp, "tp": sibling}).wait_recv()
    window_branch = jnp.zeros((rows, block), F32)
    for j in range(n_tp):
        window_branch = window_branch + dot(win[j], columns[0][j])
    gates[0] = gates[0] * window_branch
    for part in range(2):
        at = slice(part * half, (part + 1) * half)
        forward(lat_half[part], 3 + part)
        arrived(lat_half[part], 3 + part)
        latent_branch = jnp.zeros((half, block), F32)
        for j in range(n_tp):
            latent_branch = latent_branch + dot(lat[j, part], columns[1][j])
        out[at, :] = (gates[0, at] + gates[1, at] * latent_branch).astype(BF16)

    for which, view in enumerate((*feat_half, win_all, *lat_half)):
        sent(view, which)
    for copy in column_sends:
        copy.wait_send()

    @pl.when(sp + 1 < n_sp)
    def _():
        halo_copy.wait_send()

    def drain(k, _):
        @pl.when(z >= k)
        def _():
            for h in range(2):
                @pl.when(z + 1 < n_z)
                def _():
                    z_copy(k, h).wait_send()

                for d in range(1, n_x):
                    x_copy(k, d, h).wait_send()
                    d_copy(k, d, h, core).wait_send()

                @pl.when(k > 0)
                def _():
                    c_copy(k, h, core).wait_send()

        return 0

    lax.fori_loop(0, n_z, drain, 0)


def on_device(dims, features, norm_gain, w_query, w_key, w_value, head_sinks, w_query_latent,
              w_kv_latent, w_rope_key, query_latent_gain, kv_latent_gain, w_query_content,
              w_query_rotary, w_key_up, w_value_up, w_branch_window, w_branch_latent,
              w_gate_window, w_gate_latent):
    n_sp, n_tp, n_x = dims
    n_z, n_y = n_sp // n_x, n_tp // 2
    rows, block = features.shape
    width = norm_gain.shape[0]
    latent = w_kv_latent.shape[1]
    lat_heads = w_key_up.shape[1] // NOPE
    half_width = ROPE // 2
    entry = lax.rem(jnp.arange(ROPE, dtype=jnp.int32), half_width).astype(F32)
    frequency = (THETA ** (-entry / half_width))[None, :]
    weights = (w_kv_latent, w_rope_key.T, w_key, w_value, w_query, w_query_latent, w_query_content,
               w_query_rotary, w_key_up, w_value_up, w_gate_window, w_gate_latent)
    branches = (w_branch_window, w_branch_latent)
    vmem = pl.BlockSpec(memory_space=pltpu.VMEM)
    hbm = pl.BlockSpec(memory_space=pl.ANY)
    dma = pltpu.SemaphoreType.DMA
    return pl.pallas_call(
        functools.partial(kernel, dims),
        out_shape=jax.ShapeDtypeStruct((rows, block), BF16),
        in_specs=[hbm, vmem, pl.BlockSpec(memory_space=pltpu.SMEM), vmem, vmem, vmem]
        + [hbm] * (len(weights) + 2),
        out_specs=vmem,
        scratch_shapes=[
            pltpu.VMEM((n_tp, 2, rows // 2, block), BF16),
            pltpu.VMEM((rows, width), BF16),
            pltpu.VMEM((rows, latent), F32),
            *[pltpu.VMEM(weight.shape, BF16) for weight in weights],
            *[pltpu.VMEM((n_tp, branch.shape[0], block), BF16) for branch in branches],
            pltpu.VMEM((n_sp, 2, 2, rows // 4, latent + LANES), BF16),
            pltpu.VMEM((rows, 2 * w_key.shape[1]), BF16),
            pltpu.VMEM((WINDOW, 2 * w_key.shape[1]), BF16),
            pltpu.VMEM((rows, w_query.shape[1]), BF16),
            pltpu.VMEM((lat_heads, rows, NOPE + LANES), BF16),
            pltpu.VMEM((2, rows, block), F32),
            pltpu.VMEM((n_tp, rows, w_query.shape[1]), BF16),
            pltpu.VMEM((n_tp, 2, rows // 2, lat_heads * VDIM), BF16),
            *[pltpu.VMEM((lat_heads, rows, LANES), F32)] * 3,
            dma((len(weights),)),
            dma((2,)),
            dma((2,)),
            dma((2, n_tp)),
            dma((2, n_tp)),
            dma((2,)),
            *[dma((5, n_y))] * 4,
            dma((2, n_z + 1)),
            dma((2, n_z + 1)),
            dma((2, n_z, n_x)),
            dma((2, n_z, n_x)),
            dma((2, n_z)),
            dma((2, n_z)),
            dma((2, n_z, n_x)),
            dma((2, n_z, n_x)),
            *[pltpu.VMEM((rows, ROPE), F32)] * 2,
        ],
        compiler_params=pltpu.CompilerParams(
            collective_id=0, has_side_effects=True, vmem_limit_bytes=60 * 1024 * 1024
        ),
    )(features, norm_gain[None, :], head_sinks[None, :], query_latent_gain[None, :],
      kv_latent_gain[None, :], frequency, *weights, *branches)


def solution(mesh):
    n_sp, n_tp = mesh.shape["sp"], mesh.shape["tp"]
    n_x = 1
    while n_sp % (2 * n_x) == 0 and 8 * n_x * n_x <= n_sp:
        n_x *= 2
    return jax.shard_map(
        functools.partial(on_device, (n_sp, n_tp, n_x)),
        mesh=mesh,
        in_specs=(
            P("sp", "tp"),
            P(),
            P(None, "tp"),
            P(None, "tp"),
            P(None, "tp"),
            P("tp"),
            P(),
            P(),
            P(),
            P(),
            P(),
            P(None, "tp"),
            P(None, "tp"),
            P(None, "tp"),
            P(None, "tp"),
            P("tp", None),
            P("tp", None),
            P(None, "tp"),
            P(None, "tp"),
        ),
        out_specs=P("sp", "tp"),
        check_vma=False,
    )
```
